32 devices in a mesh: fs: 16 (over z, y, x), tp: 2 (over core).
Axes of the slice: x: 2, y: 2, z: 4, core: 2. Of those that a mesh axis runs over, the one named last changes fastest.
Arguments:
- tokens: bfloat16 [3072, 2048], P('fs'), may hold values from -6 to 6
- route_ids: int32 [3072, 2], P('fs'), may hold values from 0 to 7, all different within a row; in each aligned block of 192 rows (0 to 191, 192 to 383, ...) at most 96 rows name the same one
- route_logits: float32 [3072, 2], P('fs'), may hold values from -6 to 6
- norm_gain: float32 [2048], P('fs'), may hold values from 0.1 to 1.9
- gate_weight: float32 [8, 2048, 2048], P(None, 'fs', 'tp'), may hold values from -0.125 to 0.125
- up_weight: float32 [8, 2048, 2048], P(None, 'fs', 'tp'), may hold values from -0.125 to 0.125
- down_weight: float32 [8, 2048, 2048], P(None, 'fs', 'tp'), may hold values from -0.125 to 0.125
Outputs:
- mixed: bfloat16 [3072, 2048], P('fs')
- gate_copies: bfloat16 [16, 2048, 2048], P('fs', None, 'tp')
- up_copies: bfloat16 [16, 2048, 2048], P('fs', None, 'tp')
- down_copies: bfloat16 [16, 2048, 2048], P('fs', None, 'tp')
The draws below stay inside these ranges and needn't reach their ends.
Inputs may be any that keep to these rules, and one draw needn't show every extreme that they name: `route_ids`: each row names 2 different experts. Among the rows of one index of fs no expert is named by more than 96 rows, a bound that some of them reach.
All inputs are finite; a program needn't handle non-finite values.
Results may differ from the reference program's by a relative error of at most 0.014.
Values may be sent and summed in bfloat16 or wider, within the bound.
A program may use at most 128 MiB of HBM per device.

```python
import math
import jax
import jax.numpy as jnp
import numpy as np
from jax import lax

D = 2048
FF = 2048
EXPERTS = 8
TOP = 2
TOK_DEV = 192
CAP = 96
TOKENS = 3072
N_FS = 16
N_TP = 2


def levels(key, extent, split, low, high):
    def one(dim, blocks):
        steps = jax.random.uniform(jax.random.fold_in(jax.random.fold_in(key, 6), dim), (blocks,), jnp.float32, low / len(split), high / len(split))
        return jnp.repeat(jnp.exp(steps), extent[dim] // blocks).reshape((-1,) + (1,) * (len(extent) - dim - 1))

    level = one(*split[0])
    for cut in split[1:]:
        level = level * one(*cut)
    return level


def deal_out(rng, own, number, rows, number_of, top, most, lean):
    ranking = jax.random.permutation(rng, number_of)
    packed, usual = load_shares(number_of, rows * top, most, lean, True), load_shares(number_of, rows * top, most, lean, False)
    places = jnp.arange(number_of)

    def named(tallies, rotation):
        used = int((tallies > 0).sum())
        fixed = max(1, used // 4)
        moved = fixed + (places - fixed + rotation * (used - fixed)) % max(1, number_of - fixed)
        return jnp.zeros((number_of,), jnp.int32).at[ranking[jnp.where(places < fixed, places, moved)]].set(jnp.asarray(tallies, jnp.int32))

    tallies = jnp.where(number % 4 == 0, named(packed, number // 4), named(usual, number - number // 4 - 1))
    mixed = jax.random.permutation(jax.random.fold_in(own, 3), number_of)
    donor, sink = mixed[0:number_of // 2 * 2:2], mixed[1:number_of // 2 * 2:2]
    margin = jnp.minimum(tallies[donor] - 1, most - tallies[sink]) // 2
    margin = jnp.where((donor == ranking[0]) | (sink == ranking[0]) | (tallies[sink] == 0), 0, jnp.maximum(margin, 0))
    moved = jax.random.randint(jax.random.fold_in(own, 4), (number_of // 2,), 0, 1 << 20) % (margin + 1)
    tallies = tallies.at[donor].add(-moved).at[sink].add(moved)
    labels = jnp.searchsorted(jnp.cumsum(tallies), jnp.arange(rows * top), side="right").astype(jnp.int32)
    grid = labels.reshape(top, rows).T
    grid = grid[jax.random.permutation(jax.random.fold_in(own, 1), rows)]
    rotation = jax.random.randint(jax.random.fold_in(own, 2), (rows, 1), 0, top)
    return jnp.take_along_axis(grid, (jnp.arange(top)[None, :] + rotation) % top, axis=1)


def load_shares(amount, total, reach, skew, full):
    weights = [(1 << 20) // math.isqrt(rank ** skew) + 1 for rank in range(1, amount + 1)]
    largest = reach if full else min(reach, max(-(-total // amount), total * weights[0] // sum(weights)))
    least = 1 if total - largest >= amount - 1 else 0
    given, rest = [largest] + [least] * (amount - 1), total - largest - least * (amount - 1)
    while rest > 0:
        candidates = [i for i in range(1, amount) if given[i] < largest] or [i for i in range(1, amount) if given[i] < reach]
        pool, left = sum([weights[i] for i in candidates]), rest
        for i in candidates:
            more = min(reach - given[i], max(1, left * weights[i] // pool), rest)
            given[i] = given[i] + more
            rest = rest - more
    return np.array(given)


def centred(stream_key, extent, deviation, limit, cuts=(), held_as=jnp.bfloat16):
    result = deviation * jax.random.normal(stream_key, extent, jnp.float32)
    if cuts:
        result = result * levels(stream_key, extent, cuts, -0.22, 0.18)
    return jnp.clip(result, -limit, limit).astype(held_as)


def setup_inputs(seed: int = 0) -> dict:
    seeds = jax.random.split(jax.random.key(seed), 8)
    tokens = centred(seeds[0], (TOKENS, D), 1.0, 6.0, ((0, 16),))
    route_ids_keys = jax.random.split(jax.random.fold_in(seeds[1], 1), TOKENS // TOK_DEV)
    route_ids_turns = jax.random.permutation(jax.random.fold_in(seeds[1], 3), TOKENS // TOK_DEV)
    route_ids = jax.vmap(lambda own, number: deal_out(jax.random.fold_in(seeds[1], 2), own, number, TOK_DEV, EXPERTS, TOP, CAP, 1))(route_ids_keys, route_ids_turns).reshape((TOKENS, TOP))
    route_logits = centred(seeds[2], (TOKENS, TOP), 1.5, 6.0, ((0, 16),), jnp.float32)
    norm_gain = jnp.clip(1.0 + 0.18 * jax.random.normal(seeds[3], (D,), jnp.float32), 0.1, 1.9)
    gate_weight = centred(seeds[4], (EXPERTS, D, FF), D ** -0.5, 0.125, ((1, 16), (2, 2)), jnp.float32)
    up_weight = centred(seeds[5], (EXPERTS, D, FF), D ** -0.5, 0.125, ((1, 16), (2, 2)), jnp.float32)
    down_weight = centred(seeds[6], (EXPERTS, D, FF), FF ** -0.5, 0.125, ((1, 16), (2, 2)), jnp.float32)
    return dict(tokens=tokens, route_ids=route_ids, route_logits=route_logits, norm_gain=norm_gain, gate_weight=gate_weight, up_weight=up_weight, down_weight=down_weight)


def expert_rows(rows, gate_matrix, up_matrix, down_matrix):
    gate_act = jnp.dot(rows, gate_matrix, preferred_element_type=jnp.float32)
    up_act = jnp.dot(rows, up_matrix, preferred_element_type=jnp.float32)
    hidden = (jax.nn.silu(gate_act) * up_act).astype(jnp.bfloat16)
    row_count = rows.shape[0]
    blocks = hidden.reshape(row_count, N_TP, FF // N_TP).astype(jnp.float32)
    down_blocks = down_matrix.reshape(D, N_TP, FF // N_TP).astype(jnp.float32)
    partial_value = jnp.einsum('rbf,dbf->brd', blocks, down_blocks)
    rounded = lax.optimization_barrier(partial_value.astype(jnp.bfloat16))
    return lax.optimization_barrier(jnp.sum(rounded.astype(jnp.float32), axis=0)).astype(jnp.bfloat16)

def reference(tokens, route_ids, route_logits, norm_gain, gate_weight, up_weight, down_weight):
    copies = N_FS // EXPERTS
    folded_gate = (norm_gain[None, :, None] * gate_weight).astype(jnp.bfloat16)
    folded_up = (norm_gain[None, :, None] * up_weight).astype(jnp.bfloat16)
    down_cast = down_weight.astype(jnp.bfloat16)
    gate_copies = jnp.repeat(folded_gate, copies, axis=0)
    up_copies = jnp.repeat(folded_up, copies, axis=0)
    down_copies = jnp.repeat(down_cast, copies, axis=0)
    values = tokens.astype(jnp.float32)
    center = lax.optimization_barrier(jnp.mean(values, axis=1, keepdims=True))
    spread = lax.optimization_barrier(jnp.mean(jnp.square(values - center), axis=1, keepdims=True))
    normed = ((values - center) * lax.rsqrt(spread + 1e-06)).astype(jnp.bfloat16)
    per_source = route_ids.reshape(N_FS, TOK_DEV * TOP)
    onehot_table = (per_source[:, :, None] == jnp.arange(EXPERTS, dtype=jnp.int32)[None, None, :]).astype(jnp.int32)
    before = jnp.cumsum(onehot_table, axis=1) - onehot_table
    order_rank = lax.optimization_barrier(jnp.sum(before * onehot_table, axis=2))
    source = jnp.arange(N_FS, dtype=jnp.int32)[:, None]
    position = source * CAP + order_rank
    owners = source * TOK_DEV + jnp.arange(TOK_DEV * TOP, dtype=jnp.int32)[None, :] // TOP
    slot_token = jnp.full((EXPERTS, N_FS * CAP), TOKENS, jnp.int32).at[per_source, position].set(owners)
    padded = jnp.concatenate([normed, jnp.zeros((1, D), jnp.bfloat16)], axis=0)

    def one_expert(index):
        rows = padded[slot_token[index]]
        return expert_rows(rows, folded_gate[index], folded_up[index], down_cast[index])
    results = lax.map(one_expert, jnp.arange(EXPERTS, dtype=jnp.int32))
    picked = results[per_source, position].reshape(TOKENS, TOP, D).astype(jnp.float32)
    first_weight = jax.nn.sigmoid(route_logits[:, 0] - route_logits[:, 1])
    second_weight = jax.nn.sigmoid(route_logits[:, 1] - route_logits[:, 0])
    mixed = (first_weight[:, None] * picked[:, 0] + second_weight[:, None] * picked[:, 1]).astype(jnp.bfloat16)
    return (mixed, gate_copies, up_copies, down_copies)
```

```python
import functools

import jax
import jax.numpy as jnp
from jax import lax
from jax.experimental import pallas as pl
from jax.experimental.pallas import tpu as pltpu
from jax.sharding import PartitionSpec as P

CAP = 96
MESH = pl.DeviceIdType.MESH
BF16 = jnp.bfloat16
F32 = jnp.float32


def handoff(
    experts,
    copies,
    tps,
    tok,
    gain,
    gate_in,
    up_in,
    down_in,
    gate_out,
    up_out,
    down_out,
    back_out,
    stage,
    send,
    full,
    rows_in,
    hidden,
    part,
    part_in,
    share,
    back,
    load_sem,
    w_send,
    w_recv,
    r_send,
    r_recv,
    t_send,
    t_recv,
    tx_send,
    tx_recv,
    p_send,
    p_recv,
    b_send,
    b_recv,
    bx_send,
    bx_recv,
    out_sem,
    tok_sem,
):
    shard, cols = stage.shape[2], stage.shape[3]
    width = rows_in.shape[1]
    block = tok.shape[1]
    chunk_f = min(256, cols)
    chunk_w = min(256, block)
    n_f, n_w = cols // chunk_f, block // chunk_w
    me = lax.axis_index("fs")
    tp = lax.axis_index("tp")
    group = lax.div(me, copies)
    lane = lax.rem(me, copies)
    weights = (gate_in, up_in, down_in)
    outs = (gate_out, up_out, down_out)

    def ahead(d):
        return lax.rem(group + d, experts)

    def behind(d):
        return lax.rem(group + experts - d, experts)

    def twin(c):
        return lax.rem(lane + c, copies)

    def mate(p):
        return lax.rem(tp + p, tps)

    def slots(e):
        return pl.ds(pl.multiple_of(e * CAP, 32), CAP)

    def own_cols(q, j=0, size=block):
        return pl.ds(pl.multiple_of(q * block + j * chunk_w, 128), size)

    def shard_rows(g, c):
        return pl.ds(pl.multiple_of((g * copies + c) * shard, 32), shard)

    def loop(lo, hi, body):
        def step(i, carry):
            body(i)
            return carry

        lax.fori_loop(lo, hi, step, 0)

    def remote(src, dst, s_sem, r_sem, fs_to, tp_to):
        return pltpu.make_async_remote_copy(
            src_ref=src,
            dst_ref=dst,
            send_sem=s_sem,
            recv_sem=r_sem,
            device_id=(fs_to, tp_to),
            device_id_type=MESH,
        )

    def load(m, h):
        return pltpu.make_async_copy(weights[m].at[h], stage.at[m, h], load_sem.at[m, h])

    def direct(m, h, s):
        return remote(
            send.at[m, h],
            full.at[m, shard_rows(s, lane)],
            w_send.at[m, h],
            w_recv.at[m, s],
            h * copies + lane,
            tp,
        )

    def relay(m, s, c, to):
        return remote(
            full.at[m, shard_rows(s, c)],
            full.at[m, shard_rows(s, c)],
            r_send.at[m, s, to],
            r_recv.at[m, s, c],
            group * copies + to,
            tp,
        )

    def dispatch(h, s):
        return remote(
            tok.at[slots(h)],
            rows_in.at[slots(s), own_cols(tp)],
            t_send.at[h],
            t_recv.at[s],
            h * copies + lane,
            tp,
        )

    def spread(s, q, p):
        return remote(
            rows_in.at[slots(s), own_cols(q)],
            rows_in.at[slots(s), own_cols(q)],
            tx_send.at[s, p],
            tx_recv.at[s, p],
            me,
            mate(p),
        )

    def partial(p, j):
        where = pl.ds(pl.multiple_of(j * chunk_w, 128), chunk_w)
        return remote(
            part.at[p - 1, :, where],
            part_in.at[p - 1, :, where],
            p_send.at[p, j],
            p_recv.at[p, j],
            me,
            mate(p),
        )

    def give(s, e, j):
        where = pl.ds(pl.multiple_of(j * chunk_w, 128), chunk_w)
        return remote(
            share.at[slots(s), where],
            back.at[slots(e), own_cols(tp, j, chunk_w)],
            b_send.at[s, j],
            b_recv.at[e, j],
            s * copies + lane,
            tp,
        )

    def fan(e, q, j, p):
        return remote(
            back.at[slots(e), own_cols(q, j, chunk_w)],
            back.at[slots(e), own_cols(q, j, chunk_w)],
            bx_send.at[e, j, p],
            bx_recv.at[e, j, p],
            me,
            mate(p),
        )

    for m in range(3):
        loop(0, experts, lambda d, m=m: load(m, ahead(d)).start())
    tok_copy = pltpu.make_async_copy(
        tok.at[slots(group)], rows_in.at[slots(group), own_cols(tp)], tok_sem
    )
    tok_copy.start()

    barrier = pltpu.get_barrier_semaphore()
    for d in range(1, experts):
        pl.semaphore_signal(
            barrier, inc=1, device_id=(ahead(d) * copies + lane, tp), device_id_type=MESH
        )
    for c in range(1, copies):
        pl.semaphore_signal(
            barrier, inc=1, device_id=(group * copies + twin(c), tp), device_id_type=MESH
        )
    for p in range(1, tps):
        pl.semaphore_signal(barrier, inc=1, device_id=(me, mate(p)), device_id_type=MESH)
    pl.semaphore_wait(barrier, experts + copies + tps - 3)

    loop(1, experts, lambda d: dispatch(ahead(d), group).start())

    def rounded(m, h):
        load(m, h).wait()
        value = stage[m, h]
        if m < 2:
            value = gain[...] * value
        return value.astype(BF16)

    for m in range(3):
        full[m, shard_rows(group, lane)] = rounded(m, group)
    for m in range(3):
        def convert(d, m=m):
            send[m, ahead(d)] = rounded(m, ahead(d))

            @pl.when(d > 1)
            def _():
                direct(m, ahead(d - 1), group).start()

        loop(1, experts, convert)
        for c in range(1, copies):
            relay(m, group, lane, twin(c)).start()
        direct(m, ahead(experts - 1), group).start()

    tok_copy.wait()
    for p in range(1, tps):
        spread(group, tp, p).start()

    def spread_step(d):
        s = behind(d)
        dispatch(s, s).wait_recv()
        for p in range(1, tps):
            spread(s, tp, p).start()

    def relay_step(m, d):
        s = behind(d)
        direct(m, s, s).wait_recv()
        for c in range(1, copies):
            relay(m, s, lane, twin(c)).start()

    def relay_wait(m, s):
        for c in range(1, copies):
            relay(m, s, twin(c), lane).wait_recv()

    def out_copy(m):
        return pltpu.make_async_copy(full.at[m], outs[m].at[0], out_sem.at[m])

    loop(1, experts, spread_step)
    loop(1, experts, lambda d: relay_step(0, d))
    loop(1, experts, lambda d: relay_step(1, d))
    early = experts - n_f
    loop(1, early, lambda d: relay_step(2, d))

    def spread_wait(s):
        for p in range(1, tps):
            spread(s, mate(tps - p), p).wait_recv()

    loop(0, experts, spread_wait)
    for m in range(2):
        loop(0, experts, lambda s, m=m: relay_wait(m, s))
        out_copy(m).start()

    def gate_up(c):
        relay_step(2, early + c)
        where = pl.ds(pl.multiple_of(c * chunk_f, 128), chunk_f)
        gate = jnp.dot(rows_in[...], full[0, :, where], preferred_element_type=F32)
        up = jnp.dot(rows_in[...], full[1, :, where], preferred_element_type=F32)
        hidden[:, where] = (gate / (1.0 + jnp.exp(-gate)) * up).astype(BF16)

    loop(0, n_f, gate_up)
    loop(0, experts, lambda s: relay_wait(2, s))
    out_copy(2).start()

    def down(q, j):
        rows = full[2, own_cols(q, j, chunk_w), :]
        return lax.dot_general(
            hidden[...], rows, (((1,), (1,)), ((), ())), preferred_element_type=F32
        ).astype(BF16)

    for p in range(1, tps):
        def partial_step(j, p=p):
            where = pl.ds(pl.multiple_of(j * chunk_w, 128), chunk_w)
            part[p - 1, :, where] = down(mate(p), j)
            partial(p, j).start()

        loop(0, n_w, partial_step)

    def share_step(j):
        where = pl.ds(pl.multiple_of(j * chunk_w, 128), chunk_w)
        total = down(tp, j).astype(F32)
        for p in range(1, tps):
            partial(p, j).wait_recv()
            total = total + part_in[p - 1, :, where].astype(F32)
        share[:, where] = total.astype(BF16)
        back[slots(group), own_cols(tp, j, chunk_w)] = share[slots(group), where]
        loop(1, experts, lambda d: give(behind(d), group, j).start())
        for p in range(1, tps):
            fan(group, tp, j, p).start()

    loop(0, n_w, share_step)

    def back_step(j):
        def one(d):
            e = ahead(d)
            give(e, e, j).wait_recv()
            for p in range(1, tps):
                fan(e, tp, j, p).start()

        loop(1, experts, one)

    loop(0, n_w, back_step)

    def back_wait(j):
        def one(e):
            for p in range(1, tps):
                fan(e, mate(tps - p), j, p).wait_recv()

        loop(0, experts, one)

    loop(0, n_w, back_wait)
    last = pltpu.make_async_copy(back, back_out, tok_sem)
    last.start()

    loop(1, experts, lambda d: dispatch(ahead(d), group).wait_send())
    for m in range(3):
        loop(1, experts, lambda d, m=m: direct(m, ahead(d), group).wait_send())

        def relays(s, m=m):
            for c in range(1, copies):
                relay(m, s, lane, twin(c)).wait_send()

        loop(0, experts, relays)
        out_copy(m).wait()

    def spreads(s):
        for p in range(1, tps):
            spread(s, tp, p).wait_send()

    loop(0, experts, spreads)

    def tail(j):
        for p in range(1, tps):
            partial(p, j).wait_send()
        loop(1, experts, lambda d: give(behind(d), group, j).wait_send())

        def fans(e):
            for p in range(1, tps):
                fan(e, tp, j, p).wait_send()

        loop(0, experts, fans)

    loop(0, n_w, tail)
    last.wait()


def body(tokens, route_ids, route_logits, norm_gain, gate_weight, up_weight, down_weight):
    experts, shard, cols = gate_weight.shape
    fs_count, tps = lax.axis_size("fs"), lax.axis_size("tp")
    copies = fs_count // experts
    tok_rows, width = tokens.shape
    block = width // tps
    n_slots = experts * CAP
    depth = shard * fs_count

    values = tokens.astype(F32)
    center = jnp.mean(values, axis=1, keepdims=True)
    spread = jnp.mean(jnp.square(values - center), axis=1, keepdims=True)
    normed = ((values - center) * lax.rsqrt(spread + 1e-06)).astype(BF16)

    expert_ids = jnp.arange(experts, dtype=jnp.int32)[None, :]
    hit = [route_ids[:, k : k + 1] == expert_ids for k in range(2)]
    named = (hit[0] | hit[1]).astype(BF16)
    order = jnp.arange(tok_rows, dtype=jnp.int32)
    lower = (order[None, :] < order[:, None]).astype(BF16)
    rank = jnp.dot(lower, named, preferred_element_type=F32).astype(jnp.int32)
    place = expert_ids * CAP + rank
    slot = [jnp.sum(jnp.where(hit[k], place, 0), axis=1) for k in range(2)]
    slot_ids = jnp.arange(n_slots, dtype=jnp.int32)
    scatter = (
        (slot_ids[:, None] == slot[0][None, :]) | (slot_ids[:, None] == slot[1][None, :])
    ).astype(BF16)
    mine = lax.dynamic_slice_in_dim(normed, lax.axis_index("tp") * block, block, 1)
    tok = jnp.dot(scatter, mine, preferred_element_type=F32).astype(BF16)

    n_w = block // min(256, block)
    dma = pltpu.SemaphoreType.DMA
    anywhere = pl.BlockSpec(memory_space=pl.ANY)
    copy_shape = jax.ShapeDtypeStruct((1, depth, cols), BF16)
    gate_new, up_new, down_new, returned = pl.pallas_call(
        functools.partial(handoff, experts, copies, tps),
        out_shape=(
            copy_shape,
            copy_shape,
            copy_shape,
            jax.ShapeDtypeStruct((n_slots, width), BF16),
        ),
        in_specs=[anywhere, pl.BlockSpec(memory_space=pltpu.VMEM)] + [anywhere] * 3,
        out_specs=(anywhere,) * 4,
        scratch_shapes=[
            pltpu.VMEM((3, experts, shard, cols), F32),
            pltpu.VMEM((3, experts, shard, cols), BF16),
            pltpu.VMEM((3, depth, cols), BF16),
            pltpu.VMEM((n_slots, width), BF16),
            pltpu.VMEM((n_slots, cols), BF16),
            pltpu.VMEM((tps - 1, n_slots, block), BF16),
            pltpu.VMEM((tps - 1, n_slots, block), BF16),
            pltpu.VMEM((n_slots, block), BF16),
            pltpu.VMEM((n_slots, width), BF16),
            dma((3, experts)),
            dma((3, experts)),
            dma((3, experts)),
            dma((3, experts, copies)),
            dma((3, experts, copies)),
            dma((experts,)),
            dma((experts,)),
            dma((experts, tps)),
            dma((experts, tps)),
            dma((tps, n_w)),
            dma((tps, n_w)),
            dma((experts, n_w)),
            dma((experts, n_w)),
            dma((experts, n_w, tps)),
            dma((experts, n_w, tps)),
            dma((3,)),
            dma,
        ],
        compiler_params=pltpu.CompilerParams(
            collective_id=0, has_side_effects=True, vmem_limit_bytes=64 * 1024 * 1024 - 65536
        ),
        name="handoff",
    )(tok, norm_gain[:, None], gate_weight, up_weight, down_weight)

    picked = [
        jnp.dot(
            (slot[k][:, None] == slot_ids[None, :]).astype(BF16),
            returned,
            preferred_element_type=F32,
        )
        for k in range(2)
    ]
    first_weight = jax.nn.sigmoid(route_logits[:, 0] - route_logits[:, 1])
    second_weight = jax.nn.sigmoid(route_logits[:, 1] - route_logits[:, 0])
    mixed = (first_weight[:, None] * picked[0] + second_weight[:, None] * picked[1]).astype(BF16)
    return (mixed, gate_new, up_new, down_new)


def solution(mesh):
    return jax.shard_map(
        body,
        mesh=mesh,
        in_specs=(
            P("fs", None),
            P("fs", None),
            P("fs", None),
            P("fs"),
            P(None, "fs", "tp"),
            P(None, "fs", "tp"),
            P(None, "fs", "tp"),
        ),
        out_specs=(P("fs", None), P("fs", None, "tp"), P("fs", None, "tp"), P("fs", None, "tp")),
        check_vma=False,
    )
```

```python
import functools

import jax
import jax.numpy as jnp
from jax import lax
from jax.experimental import pallas as pl
from jax.experimental.pallas import tpu as pltpu
from jax.sharding import PartitionSpec as P

CAP = 96
STRIDE = 1
MESH = pl.DeviceIdType.MESH
BF16 = jnp.bfloat16
F32 = jnp.float32


def handoff(
    experts,
    copies,
    tps,
    tok,
    gain,
    gate_in,
    up_in,
    down_in,
    gate_out,
    up_out,
    down_out,
    back_out,
    stage,
    send,
    full,
    rows_in,
    hidden,
    part,
    part_in,
    share,
    back,
    load_sem,
    w_send,
    w_recv,
    r_send,
    r_recv,
    t_send,
    t_recv,
    tx_send,
    tx_recv,
    p_send,
    p_recv,
    b_send,
    b_recv,
    bx_send,
    bx_recv,
    out_sem,
    tok_sem,
):
    shard, cols = stage.shape[2], stage.shape[3]
    width = rows_in.shape[1]
    block = tok.shape[1]
    chunk_f = min(256, cols)
    chunk_w = width // experts
    n_f, n_w = cols // chunk_f, experts // tps
    me = lax.axis_index("fs")
    tp = lax.axis_index("tp")
    group = lax.div(me, copies)
    lane = lax.rem(me, copies)
    weights = (gate_in, up_in, down_in)
    outs = (gate_out, up_out, down_out)

    paired = experts & (experts - 1) == 0

    def ahead(d):
        if paired:
            return lax.bitwise_xor(group, lax.rem(jnp.int32(d) * STRIDE, experts))
        return lax.rem(group + d, experts)

    def behind(d):
        if paired:
            return ahead(d)
        return lax.rem(group + experts - d, experts)

    def twin(c):
        return lax.rem(lane + c, copies)

    def mate(p):
        return lax.rem(tp + p, tps)

    def slots(e):
        return pl.ds(pl.multiple_of(e * CAP, 32), CAP)

    def own_cols(q, j=0, size=block):
        return pl.ds(pl.multiple_of(q * block + j * chunk_w, 128), size)

    def shard_rows(g, c):
        return pl.ds(pl.multiple_of((g * copies + c) * shard, 32), shard)

    def loop(lo, hi, body):
        def step(i, carry):
            body(i)
            return carry

        lax.fori_loop(lo, hi, step, 0)

    def remote(src, dst, s_sem, r_sem, fs_to, tp_to):
        return pltpu.make_async_remote_copy(
            src_ref=src,
            dst_ref=dst,
            send_sem=s_sem,
            recv_sem=r_sem,
            device_id=(fs_to, tp_to),
            device_id_type=MESH,
        )

    def load(m, h):
        return pltpu.make_async_copy(weights[m].at[h], stage.at[m, h], load_sem.at[m, h])

    def direct(m, h, s):
        return remote(
            send.at[m, h],
            full.at[m, shard_rows(s, lane)],
            w_send.at[m, h],
            w_recv.at[m, s],
            h * copies + lane,
            tp,
        )

    def relay(m, s, c, to):
        return remote(
            full.at[m, shard_rows(s, c)],
            full.at[m, shard_rows(s, c)],
            r_send.at[m, s, to],
            r_recv.at[m, s, c],
            group * copies + to,
            tp,
        )

    def dispatch(h, s):
        return remote(
            tok.at[slots(h)],
            rows_in.at[slots(s), own_cols(tp)],
            t_send.at[h],
            t_recv.at[s],
            h * copies + lane,
            tp,
        )

    def spread(s, q, p):
        return remote(
            rows_in.at[slots(s), own_cols(q)],
            rows_in.at[slots(s), own_cols(q)],
            tx_send.at[s, p],
            tx_recv.at[s, p],
            me,
            mate(p),
        )

    def features(e):
        return pl.ds(pl.multiple_of(e * chunk_w, 128), chunk_w)

    def partial(e, q):
        owner, j = lax.div(e, n_w), lax.rem(e, n_w)
        p = lax.rem(owner - q + tps, tps)
        return remote(
            part.at[:, features(e)],
            part_in.at[p - 1, :, features(j)],
            p_send.at[e],
            p_recv.at[p, j],
            me,
            owner,
        )

    def give(s, e, j):
        where = pl.ds(pl.multiple_of(j * chunk_w, 128), chunk_w)
        return remote(
            share.at[slots(s), where],
            back.at[slots(e), own_cols(tp, j, chunk_w)],
            b_send.at[s, j],
            b_recv.at[e, j],
            s * copies + lane,
            tp,
        )

    def fan(e, q, j, p):
        return remote(
            back.at[slots(e), own_cols(q, j, chunk_w)],
            back.at[slots(e), own_cols(q, j, chunk_w)],
            bx_send.at[e, j, p],
            bx_recv.at[e, j, p],
            me,
            mate(p),
        )

    for m in range(3):
        loop(0, experts, lambda d, m=m: load(m, ahead(d)).start())
    tok_copy = pltpu.make_async_copy(
        tok.at[slots(group)], rows_in.at[slots(group), own_cols(tp)], tok_sem
    )
    tok_copy.start()

    barrier = pltpu.get_barrier_semaphore()
    for d in range(1, experts):
        pl.semaphore_signal(
            barrier, inc=1, device_id=(ahead(d) * copies + lane, tp), device_id_type=MESH
        )
    for c in range(1, copies):
        pl.semaphore_signal(
            barrier, inc=1, device_id=(group * copies + twin(c), tp), device_id_type=MESH
        )
    for p in range(1, tps):
        pl.semaphore_signal(barrier, inc=1, device_id=(me, mate(p)), device_id_type=MESH)
    pl.semaphore_wait(barrier, experts + copies + tps - 3)

    loop(1, experts, lambda d: dispatch(ahead(d), group).start())

    def rounded(m, h):
        load(m, h).wait()
        value = stage[m, h]
        if m < 2:
            value = gain[...] * value
        return value.astype(BF16)

    for m in range(3):
        full[m, shard_rows(group, lane)] = rounded(m, group)
    for m in range(3):
        def convert(d, m=m):
            send[m, ahead(d)] = rounded(m, ahead(d))

            @pl.when(d > 1)
            def _():
                direct(m, ahead(d - 1), group).start()

        loop(1, experts, convert)
        for c in range(1, copies):
            relay(m, group, lane, twin(c)).start()
        direct(m, ahead(experts - 1), group).start()

    tok_copy.wait()
    for p in range(1, tps):
        spread(group, tp, p).start()

    def spread_step(d):
        s = behind(d)
        dispatch(s, s).wait_recv()
        for p in range(1, tps):
            spread(s, tp, p).start()

    def relay_step(m, d):
        s = behind(d)
        direct(m, s, s).wait_recv()
        for c in range(1, copies):
            relay(m, s, lane, twin(c)).start()

    def relay_wait(m, s):
        for c in range(1, copies):
            relay(m, s, twin(c), lane).wait_recv()

    def out_copy(m):
        return pltpu.make_async_copy(full.at[m], outs[m].at[0], out_sem.at[m])

    loop(1, experts, spread_step)
    loop(1, experts, lambda d: relay_step(0, d))
    loop(1, experts, lambda d: relay_step(1, d))
    def spread_wait(s):
        for p in range(1, tps):
            spread(s, mate(tps - p), p).wait_recv()

    loop(0, experts, spread_wait)
    for m in range(2):
        loop(0, experts, lambda s, m=m: relay_wait(m, s))
        out_copy(m).start()

    def gate_up(c):
        @pl.when(c < experts - 1)
        def _():
            relay_step(2, 1 + c)

        where = pl.ds(pl.multiple_of(c * chunk_f, 128), chunk_f)
        gate = jnp.dot(rows_in[...], full[0, :, where], preferred_element_type=F32)
        up = jnp.dot(rows_in[...], full[1, :, where], preferred_element_type=F32)
        hidden[:, where] = (gate / (1.0 + jnp.exp(-gate)) * up).astype(BF16)

    loop(0, n_f, gate_up)
    def add_up(e):
        @pl.when(lax.div(e, n_w) == tp)
        def _():
            j = lax.rem(e, n_w)
            total = part[:, features(e)].astype(F32)
            for p in range(1, tps):
                partial(e, mate(tps - p)).wait_recv()
                total = total + part_in[p - 1, :, features(j)].astype(F32)
            share[:, features(j)] = total.astype(BF16)
            back[slots(group), features(e)] = share[slots(group), features(j)]
            loop(1, experts, lambda d: give(behind(d), group, j).start())
            for p in range(1, tps):
                fan(group, tp, j, p).start()

    def down_step(d):
        e = behind(d)

        @pl.when(d + n_f < experts - 1)
        def _():
            relay_step(2, d + n_f + 1)

        relay_wait(2, e)
        part[:, features(e)] = lax.dot_general(
            hidden[...],
            full[2, features(e), :],
            (((1,), (1,)), ((), ())),
            preferred_element_type=F32,
        ).astype(BF16)

        @pl.when(lax.div(e, n_w) != tp)
        def _():
            partial(e, tp).start()

        @pl.when(d > 0)
        def _():
            add_up(behind(d - 1))

    loop(0, experts, down_step)
    out_copy(2).start()
    add_up(behind(experts - 1))

    def back_step(j):
        def one(d):
            e = ahead(d)
            give(e, e, j).wait_recv()
            for p in range(1, tps):
                fan(e, tp, j, p).start()

        loop(1, experts, one)

    loop(0, n_w, back_step)

    def back_wait(j):
        def one(e):
            for p in range(1, tps):
                fan(e, mate(tps - p), j, p).wait_recv()

        loop(0, experts, one)

    loop(0, n_w, back_wait)
    last = pltpu.make_async_copy(back, back_out, tok_sem)
    last.start()

    loop(1, experts, lambda d: dispatch(ahead(d), group).wait_send())
    for m in range(3):
        loop(1, experts, lambda d, m=m: direct(m, ahead(d), group).wait_send())

        def relays(s, m=m):
            for c in range(1, copies):
                relay(m, s, lane, twin(c)).wait_send()

        loop(0, experts, relays)
        out_copy(m).wait()

    def spreads(s):
        for p in range(1, tps):
            spread(s, tp, p).wait_send()

    loop(0, experts, spreads)

    def part_sent(e):
        @pl.when(lax.div(e, n_w) != tp)
        def _():
            partial(e, tp).wait_send()

    loop(0, experts, part_sent)

    def tail(j):
        loop(1, experts, lambda d: give(behind(d), group, j).wait_send())

        def fans(e):
            for p in range(1, tps):
                fan(e, tp, j, p).wait_send()

        loop(0, experts, fans)

    loop(0, n_w, tail)
    last.wait()


def body(tokens, route_ids, route_logits, norm_gain, gate_weight, up_weight, down_weight):
    experts, shard, cols = gate_weight.shape
    fs_count, tps = lax.axis_size("fs"), lax.axis_size("tp")
    copies = fs_count // experts
    tok_rows, width = tokens.shape
    block = width // tps
    n_slots = experts * CAP
    depth = shard * fs_count

    values = tokens.astype(F32)
    center = jnp.mean(values, axis=1, keepdims=True)
    spread = jnp.mean(jnp.square(values - center), axis=1, keepdims=True)
    normed = ((values - center) * lax.rsqrt(spread + 1e-06)).astype(BF16)

    expert_ids = jnp.arange(experts, dtype=jnp.int32)[None, :]
    hit = [route_ids[:, k : k + 1] == expert_ids for k in range(2)]
    named = (hit[0] | hit[1]).astype(BF16)
    order = jnp.arange(tok_rows, dtype=jnp.int32)
    lower = (order[None, :] < order[:, None]).astype(BF16)
    rank = jnp.dot(lower, named, preferred_element_type=F32).astype(jnp.int32)
    place = expert_ids * CAP + rank
    slot = [jnp.sum(jnp.where(hit[k], place, 0), axis=1) for k in range(2)]
    slot_ids = jnp.arange(n_slots, dtype=jnp.int32)
    scatter = (
        (slot_ids[:, None] == slot[0][None, :]) | (slot_ids[:, None] == slot[1][None, :])
    ).astype(BF16)
    mine = lax.dynamic_slice_in_dim(normed, lax.axis_index("tp") * block, block, 1)
    tok = jnp.dot(scatter, mine, preferred_element_type=F32).astype(BF16)

    n_w = experts // tps
    dma = pltpu.SemaphoreType.DMA
    anywhere = pl.BlockSpec(memory_space=pl.ANY)
    copy_shape = jax.ShapeDtypeStruct((1, depth, cols), BF16)
    gate_new, up_new, down_new, returned = pl.pallas_call(
        functools.partial(handoff, experts, copies, tps),
        out_shape=(
            copy_shape,
            copy_shape,
            copy_shape,
            jax.ShapeDtypeStruct((n_slots, width), BF16),
        ),
        in_specs=[anywhere, pl.BlockSpec(memory_space=pltpu.VMEM)] + [anywhere] * 3,
        out_specs=(anywhere,) * 4,
        scratch_shapes=[
            pltpu.VMEM((3, experts, shard, cols), F32),
            pltpu.VMEM((3, experts, shard, cols), BF16),
            pltpu.VMEM((3, depth, cols), BF16),
            pltpu.VMEM((n_slots, width), BF16),
            pltpu.VMEM((n_slots, cols), BF16),
            pltpu.VMEM((n_slots, width), BF16),
            pltpu.VMEM((tps - 1, n_slots, block), BF16),
            pltpu.VMEM((n_slots, block), BF16),
            pltpu.VMEM((n_slots, width), BF16),
            dma((3, experts)),
            dma((3, experts)),
            dma((3, experts)),
            dma((3, experts, copies)),
            dma((3, experts, copies)),
            dma((experts,)),
            dma((experts,)),
            dma((experts, tps)),
            dma((experts, tps)),
            dma((experts,)),
            dma((tps, n_w)),
            dma((experts, n_w)),
            dma((experts, n_w)),
            dma((experts, n_w, tps)),
            dma((experts, n_w, tps)),
            dma((3,)),
            dma,
        ],
        compiler_params=pltpu.CompilerParams(
            collective_id=0, has_side_effects=True, vmem_limit_bytes=64 * 1024 * 1024 - 65536
        ),
        name="handoff",
    )(tok, norm_gain[:, None], gate_weight, up_weight, down_weight)

    picked = [
        jnp.dot(
            (slot[k][:, None] == slot_ids[None, :]).astype(BF16),
            returned,
            preferred_element_type=F32,
        )
        for k in range(2)
    ]
    first_weight = jax.nn.sigmoid(route_logits[:, 0] - route_logits[:, 1])
    second_weight = jax.nn.sigmoid(route_logits[:, 1] - route_logits[:, 0])
    mixed = (first_weight[:, None] * picked[0] + second_weight[:, None] * picked[1]).astype(BF16)
    return (mixed, gate_new, up_new, down_new)


def solution(mesh):
    return jax.shard_map(
        body,
        mesh=mesh,
        in_specs=(
            P("fs", None),
            P("fs", None),
            P("fs", None),
            P("fs"),
            P(None, "fs", "tp"),
            P(None, "fs", "tp"),
            P(None, "fs", "tp"),
        ),
        out_specs=(P("fs", None), P("fs", None, "tp"), P("fs", None, "tp"), P("fs", None, "tp")),
        check_vma=False,
    )
```
